32 devices in a mesh: grp: 2 (over x), ep: 8 (over z, y), tp: 2 (over core).
Axes of the slice: x: 2, y: 2, z: 4, core: 2. Of those that a mesh axis runs over, the one named last changes fastest.
Arguments:
- tokens: bfloat16 [3072, 2048], P(('grp', 'ep'), 'tp'), parts along dimension 0, may hold values from -10 to 10
- gain_in: float32 [2048], replicated, may hold values from 0.1 to 1.9
- gain_out: float32 [2048], replicated, may hold values from 0.1 to 1.9
- expert_ids: int32 [3072, 2], P(('grp', 'ep')), parts along dimension 0, may hold values from 0 to 3, all different within a row; in each aligned block of 192 rows (0 to 191, 192 to 383, ...) at most 144 rows name the same one
- route_weight: float32 [3072, 2], P(('grp', 'ep')), parts along dimension 0, may hold values from 0.1 to 1
- gate_weight: bfloat16 [8, 2048, 1792], P('ep', None, 'tp'), may hold values from -0.125 to 0.125
- up_weight: bfloat16 [8, 2048, 1792], P('ep', None, 'tp'), may hold values from -0.125 to 0.125
- down_weight: bfloat16 [8, 1792, 2048], P('ep', 'tp'), may hold values from -1 to 1
Outputs:
- layer_out: bfloat16 [3072, 2048], P(('grp', 'ep'), 'tp'), parts along dimension 0
The draws below stay inside these ranges and needn't reach their ends.
There are 2 independent parts, one for each index of `grp`. The reference program is written for one: setup_inputs(seed, part) draws one part's arguments, and reference() takes and returns one part's arrays. A program takes and returns all parts, laid end to end along the dimension named above; an argument that names none is the same for every part. Nothing has to cross between parts.
Inputs may be any that keep to these rules, and one draw needn't show every extreme that they name: `expert_ids`: each row names 2 different experts. Among the tokens of one index of ep no expert is named more than 144 times, a bound that some block reaches.
All inputs are finite; a program needn't handle non-finite values.
Results may differ from the reference program's by a relative error of at most 0.0077.
Values may be sent and summed in bfloat16 or wider, within the bound.
No kernel may reach another device: no remote copies, remote signals or barrier semaphores. Data moves between devices by JAX's collectives and lax.ppermute only.
A program may use at most 64 MiB of HBM per device.

```python
import math
import jax
import jax.numpy as jnp
import numpy as np
from jax import lax

D = 2048
DE = 3584
TOP_K = 2
TOK_EP = 192
EXPERTS = 4
TOKENS = 1536
CAP = 144
N_EP = 8


def column_factors(key):
    key_low, key_high, key_flip = jax.random.split(jax.random.fold_in(key, 11), 3)
    lowest = jax.random.uniform(key_low, (), jnp.float32, 0.35, 0.55)
    highest = jax.random.uniform(key_high, (), jnp.float32, 1.7, 2.4)
    flipped = jax.random.randint(key_flip, (), 0, 2) == 1
    first_half = jnp.where(flipped, highest, lowest)
    second_half = jnp.where(flipped, lowest, highest)
    return jnp.concatenate([jnp.full((D // 2,), first_half, jnp.float32), jnp.full((D - D // 2,), second_half, jnp.float32)])


def draw_tokens(key, part):
    key_base, key_rows = jax.random.split(jax.random.fold_in(key, 3))
    base = jnp.clip(jax.random.normal(key_base, (TOKENS, D), jnp.float32), -4.0, 4.0)
    return (base * column_factors(jax.random.fold_in(key, 5))[None, :]).astype(jnp.bfloat16)


def draw_down_weight(key, part):
    key_base = jax.random.fold_in(key, 7)
    base = jnp.clip(jax.random.normal(key_base, (2 * EXPERTS, DE // 2, D), jnp.float32), -4.0, 4.0)
    base = base * DE ** (-0.5)
    return (base * column_factors(jax.random.fold_in(key, 9))[None, None, :]).astype(jnp.bfloat16)


def block_levels(rng, shape, pieces, low, top_value):
    factor_of, own = 1.0, jax.random.fold_in(rng, 6)
    for position, blocks in pieces:
        steps = jnp.exp(jax.random.uniform(jax.random.fold_in(own, position), (blocks,), jnp.float32, low / len(pieces), top_value / len(pieces)))
        factor_of = factor_of * jnp.repeat(steps, shape[position] // blocks).reshape([-1 if axis == position else 1 for axis in range(len(shape))])
    return factor_of


def routed_block(rng, own, number, rows, count, top, bound, slope):
    ranking = jax.random.permutation(rng, count)
    heavy_load, usual = portions_of(count, rows * top, bound, slope, True), portions_of(count, rows * top, bound, slope, False)
    places = jnp.arange(count)

    def named(sizes, offset_by):
        used = int((sizes > 0).sum())
        fixed = max(1, used // 4)
        moved = fixed + (places - fixed + offset_by * (used - fixed)) % max(1, count - fixed)
        return jnp.zeros((count,), jnp.int32).at[ranking[jnp.where(places < fixed, places, moved)]].set(jnp.asarray(sizes, jnp.int32))

    sizes = jnp.where(number % 4 == 0, named(heavy_load, number // 4), named(usual, number - number // 4 - 1))
    mixed = jax.random.permutation(jax.random.fold_in(own, 3), count)
    source_of, sink = mixed[0:count // 2 * 2:2], mixed[1:count // 2 * 2:2]
    room = jnp.minimum(sizes[source_of] - 1, bound - sizes[sink]) // 2
    room = jnp.where((source_of == ranking[0]) | (sink == ranking[0]) | (sizes[sink] == 0), 0, jnp.maximum(room, 0))
    moved = jax.random.randint(jax.random.fold_in(own, 4), (count // 2,), 0, 1 << 20) % (room + 1)
    sizes = sizes.at[source_of].add(-moved).at[sink].add(moved)
    labels = jnp.searchsorted(jnp.cumsum(sizes), jnp.arange(rows * top), side="right").astype(jnp.int32)
    table = labels.reshape(top, rows).T
    table = table[jax.random.permutation(jax.random.fold_in(own, 1), rows)]
    offset_by = jax.random.randint(jax.random.fold_in(own, 2), (rows, 1), 0, top)
    return jnp.take_along_axis(table, (jnp.arange(top)[None, :] + offset_by) % top, axis=1)


def portions_of(amount, total, bound, skew, full):
    weights = [(1 << 20) // math.isqrt(rank ** skew) + 1 for rank in range(1, amount + 1)]
    largest = bound if full else min(bound, max(-(-total // amount), total * weights[0] // sum(weights)))
    least = 1 if total - largest >= amount - 1 else 0
    counts, surplus = [largest] + [least] * (amount - 1), total - largest - least * (amount - 1)
    while surplus > 0:
        free = [i for i in range(1, amount) if counts[i] < largest] or [i for i in range(1, amount) if counts[i] < bound]
        pool, budget = sum([weights[i] for i in free]), surplus
        for i in free:
            more = min(bound - counts[i], max(1, budget * weights[i] // pool), surplus)
            counts[i] = counts[i] + more
            surplus = surplus - more
    return np.array(counts)


def scatter_about(rng, dims, deviation, limit, cuts=(), kind=jnp.bfloat16):
    result = jax.random.normal(rng, dims, jnp.float32) * deviation
    if len(cuts) > 0:
        result = block_levels(rng, dims, cuts, -0.22, 0.18) * result
    return jnp.clip(result, min=-limit, max=limit).astype(kind)


def setup_inputs(seed: int = 0, part: int = 0) -> dict:
    seeds = jax.random.split(jax.random.key(seed), 9)
    own_keys = jax.random.split(jax.random.fold_in(seeds[8], part), 9)
    tokens = draw_tokens(jax.random.fold_in(jax.random.fold_in(seeds[8], part), 71), part)
    gain_in = jnp.clip(1.0 + 0.18 * jax.random.normal(seeds[1], (D,), jnp.float32), 0.1, 1.9)
    gain_out = jnp.clip(1.0 + 0.18 * jax.random.normal(seeds[2], (D,), jnp.float32), 0.1, 1.9)
    expert_ids_keys = jax.random.split(jax.random.fold_in(own_keys[3], 1), TOKENS // TOK_EP)
    expert_ids_turns = jax.random.permutation(jax.random.fold_in(own_keys[3], 3), TOKENS // TOK_EP)
    expert_ids = jax.vmap(lambda own, number: routed_block(jax.random.fold_in(own_keys[3], 2), own, number, TOK_EP, EXPERTS, TOP_K, CAP, 2))(expert_ids_keys, expert_ids_turns).reshape((TOKENS, TOP_K))
    route_weight = jnp.clip(0.1 + 0.9 * jax.random.uniform(own_keys[4], (TOKENS, TOP_K), jnp.float32) ** block_levels(own_keys[4], (TOKENS, TOP_K), ((0, 8),), -0.2, 0.2), 0.1, 1.0)
    gate_weight = scatter_about(seeds[5], (2 * EXPERTS, D, DE // 2), D ** -0.5, 0.125, ((0, 8), (2, 2)))
    up_weight = scatter_about(seeds[6], (2 * EXPERTS, D, DE // 2), D ** -0.5, 0.125, ((0, 8), (2, 2)))
    down_weight = draw_down_weight(jax.random.fold_in(seeds[8], 71), part)
    return dict(tokens=tokens, gain_in=gain_in, gain_out=gain_out, expert_ids=expert_ids, route_weight=route_weight, gate_weight=gate_weight, up_weight=up_weight, down_weight=down_weight)


norm_eps = 1e-06

def expert_rows(items):
    gathered, gate_pair, up_pair, down_pair = items
    quarter = gate_pair.shape[2] // 2
    rows_float = gathered.astype(jnp.float32)
    total = jnp.zeros((gathered.shape[0], down_pair.shape[2]), jnp.float32)
    for which_half in range(2):
        summed = jnp.zeros((gathered.shape[0], down_pair.shape[2]), jnp.float32)
        for which_core in range(2):
            start_col = which_core * quarter
            gate_pre = jnp.dot(rows_float, gate_pair[which_half, :, start_col:start_col + quarter].astype(jnp.float32), precision=lax.Precision.HIGHEST)
            up_pre = jnp.dot(rows_float, up_pair[which_half, :, start_col:start_col + quarter].astype(jnp.float32), precision=lax.Precision.HIGHEST)
            hidden = (jax.nn.silu(gate_pre) * up_pre).astype(jnp.bfloat16)
            partial_value = jnp.dot(hidden.astype(jnp.float32), down_pair[which_half, start_col:start_col + quarter, :].astype(jnp.float32), precision=lax.Precision.HIGHEST)
            partial_value = lax.optimization_barrier(partial_value.astype(jnp.bfloat16)).astype(jnp.float32)
            summed = summed + partial_value
        total = total + lax.optimization_barrier(summed.astype(jnp.bfloat16)).astype(jnp.float32)
    return total

def reference(tokens, gain_in, gain_out, expert_ids, route_weight, gate_weight, up_weight, down_weight):
    xfloat = tokens.astype(jnp.float32)
    factor = lax.rsqrt(lax.optimization_barrier(jnp.mean(xfloat * xfloat, axis=1, keepdims=True)) + norm_eps)
    normed = (xfloat * factor * gain_in).astype(jnp.bfloat16)
    copies = TOK_EP * TOP_K
    flat_ids = expert_ids.reshape(N_EP, copies).astype(jnp.int32)
    onehot = (flat_ids[:, :, None] == jnp.arange(EXPERTS, dtype=jnp.int32)[None, None, :]).astype(jnp.int32)
    before = jnp.cumsum(onehot, axis=1) - onehot
    slots = lax.optimization_barrier(jnp.sum(before * onehot, axis=2)).astype(jnp.int32)
    targets = (flat_ids * CAP + slots).astype(jnp.int32)
    source = (jnp.arange(copies, dtype=jnp.int32) // TOP_K).astype(jnp.int32)
    blocks = normed.reshape(N_EP, TOK_EP, D)

    def fill(target_rows, block):
        return jnp.zeros((EXPERTS * CAP, D), jnp.bfloat16).at[target_rows].set(block[source])
    buffers = jax.vmap(fill)(targets, blocks)
    per_expert = buffers.reshape(N_EP, EXPERTS, CAP, D).transpose(1, 0, 2, 3).reshape(EXPERTS, N_EP * CAP, D)
    gates = gate_weight.reshape(EXPERTS, 2, D, DE // 2)
    ups = up_weight.reshape(EXPERTS, 2, D, DE // 2)
    downs = down_weight.reshape(EXPERTS, 2, DE // 2, D)
    results = lax.map(expert_rows, (per_expert, gates, ups, downs))
    by_source = results.reshape(EXPERTS, N_EP, CAP, D).transpose(1, 0, 2, 3).reshape(N_EP, EXPERTS * CAP, D)

    def pick(out_rows, target_rows):
        return out_rows[target_rows]
    picked = jax.vmap(pick)(by_source, targets).reshape(TOKENS, TOP_K, D)
    routed = lax.optimization_barrier(jnp.sum(picked * route_weight[:, :, None], axis=1))
    factor_out = lax.rsqrt(lax.optimization_barrier(jnp.mean(routed * routed, axis=1, keepdims=True)) + norm_eps)
    return (routed * factor_out * gain_out).astype(jnp.bfloat16)
```

```python
import jax
import jax.numpy as jnp
from jax import lax
from jax.sharding import PartitionSpec as P

norm_eps = 1e-06


def shards(
    tokens, gain_in, gain_out, expert_ids, route_weight, gate_weight, up_weight, down_weight
):
    bf16, f32 = jnp.bfloat16, jnp.float32
    tok_rows, half_width = tokens.shape
    full_width = 2 * half_width
    ep_size = lax.axis_size("ep")
    expert_count = ep_size // 2
    picks = expert_ids.shape[1]
    capacity = tok_rows * picks * 3 // (2 * expert_count)
    pair = lax.axis_index("ep") // 2
    core = lax.axis_index("tp")
    own_cols = core * half_width
    other_cols = (1 - core) * half_width

    def swap_core(value):
        return lax.ppermute(value, "tp", [(0, 1), (1, 0)])

    def swap_half(value):
        return lax.ppermute(value, "ep", [(i, i ^ 1) for i in range(ep_size)])

    def shift_pair(value, step):
        return lax.ppermute(value, "ep", [(i, (i + 2 * step) % ep_size) for i in range(ep_size)])

    flat_ids = expert_ids.reshape(-1)
    onehot = (flat_ids[:, None] == jnp.arange(expert_count, dtype=jnp.int32)[None, :]).astype(
        jnp.int32
    )
    before = jnp.cumsum(onehot, axis=0) - onehot
    slots = jnp.sum(before * onehot, axis=1).reshape(tok_rows, picks)
    away = (expert_ids - pair + expert_count) % expert_count
    targets = away * capacity + slots

    own_float = tokens.astype(f32)
    squares = lax.psum(jnp.sum(own_float * own_float, axis=1), "tp")
    factor = lax.rsqrt(squares / full_width + norm_eps)[:, None]
    own_gain = lax.dynamic_slice_in_dim(gain_in, own_cols, half_width)
    normed = (own_float * factor * own_gain).astype(bf16)

    steps = list(range(expert_count))

    def pack(step):
        rows = jnp.arange(capacity, dtype=jnp.int32)[:, None] + step * capacity
        placing = jnp.zeros((capacity, tok_rows), bf16)
        for which in range(picks):
            placing = placing + (rows == targets[None, :, which]).astype(bf16)
        return jnp.dot(placing, normed, preferred_element_type=f32).astype(bf16)

    sent = [pack(step) for step in steps]
    mine = [sent[0]] + [shift_pair(sent[step], step) for step in steps[1:]]
    theirs = [swap_half(value) for value in mine]

    gate_own = lax.dynamic_slice_in_dim(gate_weight[0], own_cols, half_width, 0)
    gate_other = lax.dynamic_slice_in_dim(gate_weight[0], other_cols, half_width, 0)
    up_own = lax.dynamic_slice_in_dim(up_weight[0], own_cols, half_width, 0)
    up_other = lax.dynamic_slice_in_dim(up_weight[0], other_cols, half_width, 0)
    down_own = lax.dynamic_slice_in_dim(down_weight[0], own_cols, half_width, 1)
    down_other = lax.dynamic_slice_in_dim(down_weight[0], other_cols, half_width, 1)

    returned = []
    for step in steps:
        here = jnp.concatenate([mine[step], theirs[step]], axis=0)
        there = jnp.concatenate([swap_core(mine[step]), swap_core(theirs[step])], axis=0)
        gate_pre = jnp.dot(here, gate_own, preferred_element_type=f32) + jnp.dot(
            there, gate_other, preferred_element_type=f32
        )
        up_pre = jnp.dot(here, up_own, preferred_element_type=f32) + jnp.dot(
            there, up_other, preferred_element_type=f32
        )
        hidden = (jax.nn.silu(gate_pre) * up_pre).astype(bf16)
        part_other = jnp.dot(hidden, down_other, preferred_element_type=f32).astype(bf16)
        part_own = jnp.dot(hidden, down_own, preferred_element_type=f32).astype(bf16)
        half_sum = (part_own.astype(f32) + swap_core(part_other).astype(f32)).astype(bf16)
        whole = half_sum[:capacity].astype(f32) + swap_half(half_sum[capacity:]).astype(f32)
        whole = whole.astype(bf16)
        returned.append(whole if step == 0 else shift_pair(whole, -step))

    high = lax.reduce_precision(route_weight, 8, 7)
    low = (route_weight - high).astype(bf16)
    high = high.astype(bf16)
    routed = jnp.zeros((tok_rows, half_width), f32)
    for step in steps:
        cols = jnp.arange(capacity, dtype=jnp.int32)[None, :] + step * capacity
        for weight in (high, low):
            mixing = jnp.zeros((tok_rows, capacity), bf16)
            for which in range(picks):
                mixing = mixing + jnp.where(
                    cols == targets[:, which][:, None], weight[:, which][:, None], jnp.zeros((), bf16)
                )
            routed = routed + jnp.dot(mixing, returned[step], preferred_element_type=f32)
    squares_out = lax.psum(jnp.sum(routed * routed, axis=1), "tp")
    factor_out = lax.rsqrt(squares_out / full_width + norm_eps)[:, None]
    own_gain_out = lax.dynamic_slice_in_dim(gain_out, own_cols, half_width)
    return (routed * factor_out * own_gain_out).astype(bf16)


def solution(mesh):
    in_specs = (
        P(("grp", "ep"), "tp"),
        P(),
        P(),
        P(("grp", "ep"), None),
        P(("grp", "ep"), None),
        P("ep", None, "tp"),
        P("ep", None, "tp"),
        P("ep", "tp", None),
    )
    out_specs = P(("grp", "ep"), "tp")
    return jax.shard_map(shards, mesh=mesh, in_specs=in_specs, out_specs=out_specs, check_vma=False)
```

```python
import jax
import jax.numpy as jnp
from jax import lax
from jax.sharding import PartitionSpec as P

norm_eps = 1e-06


def shards(
    tokens, gain_in, gain_out, expert_ids, route_weight, gate_weight, up_weight, down_weight
):
    bf16, f32 = jnp.bfloat16, jnp.float32
    tok_rows, half_width = tokens.shape
    full_width = 2 * half_width
    ep_size = lax.axis_size("ep")
    expert_count = ep_size // 2
    picks = expert_ids.shape[1]
    capacity = tok_rows * picks * 3 // (2 * expert_count)
    pair = lax.axis_index("ep") // 2
    core = lax.axis_index("tp")
    own_cols = core * half_width
    other_cols = (1 - core) * half_width

    def swap_core(value):
        return lax.ppermute(value, "tp", [(0, 1), (1, 0)])

    def swap_half(value):
        return lax.ppermute(value, "ep", [(i, i ^ 1) for i in range(ep_size)])

    def shift_pair(value, step):
        return lax.ppermute(value, "ep", [(i, (i + 2 * step) % ep_size) for i in range(ep_size)])

    flat_ids = expert_ids.reshape(-1)
    onehot = (flat_ids[:, None] == jnp.arange(expert_count, dtype=jnp.int32)[None, :]).astype(
        jnp.int32
    )
    before = jnp.cumsum(onehot, axis=0) - onehot
    slots = jnp.sum(before * onehot, axis=1).reshape(tok_rows, picks)
    away = (expert_ids - pair + expert_count) % expert_count
    targets = away * capacity + slots

    own_float = tokens.astype(f32)
    squares = lax.psum(jnp.sum(own_float * own_float, axis=1), "tp")
    factor = lax.rsqrt(squares / full_width + norm_eps)[:, None]
    own_gain = lax.dynamic_slice_in_dim(gain_in, own_cols, half_width)
    normed = (own_float * factor * own_gain).astype(bf16)

    steps = [0]
    for near in range(1, expert_count // 2 + 1):
        steps += [near] if 2 * near == expert_count else [near, expert_count - near]

    def pack(step):
        rows = jnp.arange(capacity, dtype=jnp.int32)[:, None] + step * capacity
        placing = jnp.zeros((capacity, tok_rows), bf16)
        for which in range(picks):
            placing = placing + (rows == targets[None, :, which]).astype(bf16)
        return jnp.dot(placing, normed, preferred_element_type=f32).astype(bf16)

    sent = [pack(step) for step in steps]
    mine = [sent[0]]
    for k, step in enumerate(steps[1:], 1):
        mine.append(shift_pair(sent[k], step))
    theirs = []
    for k in range(expert_count):
        theirs.append(swap_half(mine[k]))

    gate_own = lax.dynamic_slice_in_dim(gate_weight[0], own_cols, half_width, 0)
    gate_other = lax.dynamic_slice_in_dim(gate_weight[0], other_cols, half_width, 0)
    up_own = lax.dynamic_slice_in_dim(up_weight[0], own_cols, half_width, 0)
    up_other = lax.dynamic_slice_in_dim(up_weight[0], other_cols, half_width, 0)
    down_own = lax.dynamic_slice_in_dim(down_weight[0], own_cols, half_width, 1)
    down_other = lax.dynamic_slice_in_dim(down_weight[0], other_cols, half_width, 1)

    half_sums = []
    for k in range(expert_count):
        here = jnp.concatenate([mine[k], theirs[k]], axis=0)
        there = jnp.concatenate([swap_core(mine[k]), swap_core(theirs[k])], axis=0)
        gate_pre = jnp.dot(here, gate_own, preferred_element_type=f32) + jnp.dot(
            there, gate_other, preferred_element_type=f32
        )
        up_pre = jnp.dot(here, up_own, preferred_element_type=f32) + jnp.dot(
            there, up_other, preferred_element_type=f32
        )
        hidden = (jax.nn.silu(gate_pre) * up_pre).astype(bf16)
        if k > 1:
            hidden, half_sums[k - 1] = lax.optimization_barrier((hidden, half_sums[k - 1]))
        part_other = jnp.dot(hidden, down_other, preferred_element_type=f32).astype(bf16)
        swapped = swap_core(part_other)
        part_own = jnp.dot(hidden, down_own, preferred_element_type=f32).astype(bf16)
        half_sums.append((part_own.astype(f32) + swapped.astype(f32)).astype(bf16))
    if expert_count > 1:
        half_sums[0], half_sums[-1] = lax.optimization_barrier((half_sums[0], half_sums[-1]))
    returned = []
    for k, step in enumerate(steps):
        crossed = swap_half(half_sums[k][capacity:])
        whole = (half_sums[k][:capacity].astype(f32) + crossed.astype(f32)).astype(bf16)
        returned.append(whole if step == 0 else shift_pair(whole, -step))

    high = lax.reduce_precision(route_weight, 8, 7)
    low = (route_weight - high).astype(bf16)
    high = high.astype(bf16)
    routed = jnp.zeros((tok_rows, half_width), f32)
    for k, step in enumerate(steps):
        cols = jnp.arange(capacity, dtype=jnp.int32)[None, :] + step * capacity
        for weight in (high, low):
            mixing = jnp.zeros((tok_rows, capacity), bf16)
            for which in range(picks):
                mixing = mixing + jnp.where(
                    cols == targets[:, which][:, None], weight[:, which][:, None], jnp.zeros((), bf16)
                )
            routed = routed + jnp.dot(mixing, returned[k], preferred_element_type=f32)
    squares_out = lax.psum(jnp.sum(routed * routed, axis=1), "tp")
    factor_out = lax.rsqrt(squares_out / full_width + norm_eps)[:, None]
    own_gain_out = lax.dynamic_slice_in_dim(gain_out, own_cols, half_width)
    return (routed * factor_out * own_gain_out).astype(bf16)


def solution(mesh):
    in_specs = (
        P(("grp", "ep"), "tp"),
        P(),
        P(),
        P(("grp", "ep"), None),
        P(("grp", "ep"), None),
        P("ep", None, "tp"),
        P("ep", None, "tp"),
        P("ep", "tp", None),
    )
    out_specs = P(("grp", "ep"), "tp")
    return jax.shard_map(shards, mesh=mesh, in_specs=in_specs, out_specs=out_specs, check_vma=False)
```

```python
import jax
import jax.numpy as jnp
from jax import lax
from jax.sharding import PartitionSpec as P

norm_eps = 1e-06


def shards(
    tokens, gain_in, gain_out, expert_ids, route_weight, gate_weight, up_weight, down_weight
):
    bf16, f32 = jnp.bfloat16, jnp.float32
    tok_rows, half_width = tokens.shape
    full_width = 2 * half_width
    ep_size = lax.axis_size("ep")
    expert_count = ep_size // 2
    picks = expert_ids.shape[1]
    capacity = tok_rows * picks * 3 // (2 * expert_count)
    pair = lax.axis_index("ep") // 2
    core = lax.axis_index("tp")
    own_cols = core * half_width
    other_cols = (1 - core) * half_width

    def swap_core(value):
        return lax.ppermute(value, "tp", [(0, 1), (1, 0)])

    def swap_half(value):
        return lax.ppermute(value, "ep", [(i, i ^ 1) for i in range(ep_size)])

    def shift_pair(value, step):
        return lax.ppermute(value, "ep", [(i, (i + 2 * step) % ep_size) for i in range(ep_size)])

    own_float = tokens.astype(f32)
    own_squares = jnp.sum(own_float * own_float, axis=1)
    squares = own_squares + swap_core(own_squares)

    steps = [0]
    for near in range(1, expert_count // 2 + 1):
        steps += [near] if 2 * near == expert_count else [near, expert_count - near]

    experts = (pair + jnp.array(steps, jnp.int32)) % expert_count
    named_by = expert_ids.T[None, :, :] == experts[:, None, None]
    named = jnp.any(named_by, axis=1)
    weights = jnp.sum(jnp.where(named_by, route_weight.T[None, :, :], 0.0), axis=1)
    token = jnp.arange(tok_rows, dtype=jnp.int32)
    earlier = (token[:, None] < token[None, :]).astype(bf16)
    counts = jnp.dot(named.astype(bf16), earlier, preferred_element_type=f32)
    slots = jnp.where(named, counts.astype(jnp.int32), -1)
    slot_rows = jnp.arange(capacity, dtype=jnp.int32)[:, None]

    factor = lax.rsqrt(squares / full_width + norm_eps)[:, None]
    own_gain = lax.dynamic_slice_in_dim(gain_in, own_cols, half_width)
    normed = (own_float * factor * own_gain).astype(bf16)

    def pack(k):
        placing = (slot_rows == slots[k][None, :]).astype(bf16)
        return jnp.dot(placing, normed, preferred_element_type=f32).astype(bf16)

    sent = [pack(k) for k in range(expert_count)]
    mine = [sent[0]]
    for k, step in enumerate(steps[1:], 1):
        mine.append(shift_pair(sent[k], step))
    theirs = []
    for k in range(expert_count):
        theirs.append(swap_half(mine[k]))

    gate_own = lax.dynamic_slice_in_dim(gate_weight[0], own_cols, half_width, 0)
    gate_other = lax.dynamic_slice_in_dim(gate_weight[0], other_cols, half_width, 0)
    up_own = lax.dynamic_slice_in_dim(up_weight[0], own_cols, half_width, 0)
    up_other = lax.dynamic_slice_in_dim(up_weight[0], other_cols, half_width, 0)
    down_own = lax.dynamic_slice_in_dim(down_weight[0], own_cols, half_width, 1)
    down_other = lax.dynamic_slice_in_dim(down_weight[0], other_cols, half_width, 1)

    half_sums = []
    for k in range(expert_count):
        here = jnp.concatenate([mine[k], theirs[k]], axis=0)
        there = jnp.concatenate([swap_core(mine[k]), swap_core(theirs[k])], axis=0)
        gate_pre = jnp.dot(here, gate_own, preferred_element_type=f32) + jnp.dot(
            there, gate_other, preferred_element_type=f32
        )
        up_pre = jnp.dot(here, up_own, preferred_element_type=f32) + jnp.dot(
            there, up_other, preferred_element_type=f32
        )
        hidden = (jax.nn.silu(gate_pre) * up_pre).astype(bf16)
        if k > 1:
            hidden, half_sums[k - 1] = lax.optimization_barrier((hidden, half_sums[k - 1]))
        part_other = jnp.dot(hidden, down_other, preferred_element_type=f32).astype(bf16)
        swapped = swap_core(part_other)
        part_own = jnp.dot(hidden, down_own, preferred_element_type=f32).astype(bf16)
        half_sums.append((part_own.astype(f32) + swapped.astype(f32)).astype(bf16))
    if expert_count > 1:
        half_sums[0], half_sums[-1] = lax.optimization_barrier((half_sums[0], half_sums[-1]))
    returned = []
    for k, step in enumerate(steps):
        crossed = swap_half(half_sums[k][capacity:])
        whole = (half_sums[k][:capacity].astype(f32) + crossed.astype(f32)).astype(bf16)
        returned.append(whole if step == 0 else shift_pair(whole, -step))

    high = lax.reduce_precision(weights, 8, 7)
    low = (weights - high).astype(bf16)
    high = high.astype(bf16)
    routed = jnp.zeros((tok_rows, half_width), f32)
    for k in range(expert_count):
        for weight in (high, low):
            mixing = jnp.where(slot_rows == slots[k][None, :], weight[k][None, :], jnp.zeros((), bf16))
            routed = routed + lax.dot_general(
                mixing, returned[k], (((0,), (0,)), ((), ())), preferred_element_type=f32
            )
    squares_out = lax.psum(jnp.sum(routed * routed, axis=1), "tp")
    factor_out = lax.rsqrt(squares_out / full_width + norm_eps)[:, None]
    own_gain_out = lax.dynamic_slice_in_dim(gain_out, own_cols, half_width)
    return (routed * factor_out * own_gain_out).astype(bf16)


def solution(mesh):
    in_specs = (
        P(("grp", "ep"), "tp"),
        P(),
        P(),
        P(("grp", "ep"), None),
        P(("grp", "ep"), None),
        P("ep", None, "tp"),
        P("ep", None, "tp"),
        P("ep", "tp", None),
    )
    out_specs = P(("grp", "ep"), "tp")
    return jax.shard_map(shards, mesh=mesh, in_specs=in_specs, out_specs=out_specs, check_vma=False)
```
